32 devices in a mesh: sp: 16 (over z, y, x), tp: 2 (over core).
Axes of the slice: x: 2, y: 2, z: 4, core: 2. Of those that a mesh axis runs over, the one named last changes fastest.
Arguments:
- resid: bfloat16 [4096, 2048], P(('sp', 'tp')), may hold values from -6 to 6
- queries: bfloat16 [4096, 2048], P('sp', 'tp'), may hold values from -6 to 6
- keys: bfloat16 [4096, 1024], P('sp', 'tp'), may hold values from -6 to 6
- values: bfloat16 [4096, 1024], P('sp', 'tp'), may hold values from -6 to 6
- log_gates: float32 [16, 4096], P('tp'), as said below
- documents: int32 [4096], P('sp'), may hold values from 0 to 2, never falling along the last dimension, each value on 1 to 3072 neighbouring positions
- out_weight: bfloat16 [2048, 2048], P('tp'), may hold values from -0.125 to 0.125
- attn_gain: float32 [2048], replicated, may hold values from 0.1 to 1.9
- mlp_gain: float32 [2048], replicated, may hold values from 0.1 to 1.9
- gate_weight: bfloat16 [2048, 4096], P('sp', 'tp'), may hold values from -0.125 to 0.125
- up_weight: bfloat16 [2048, 4096], P('sp', 'tp'), may hold values from -0.125 to 0.125
- down_weight: bfloat16 [4096, 2048], P('tp', 'sp'), may hold values from -0.375 to 0.375
Outputs:
- mixed: bfloat16 [4096, 2048], P(('sp', 'tp'))
The draws below stay inside these ranges and needn't reach their ends.
Inputs may be any that keep to these rules, and one draw needn't show every extreme that they name: `log_gates`: each head's row never rises from one position to the next and starts at or below 0. `documents`: document numbers never fall along the positions; one document spans exactly three quarters of the 4096 positions.
All inputs are finite; a program needn't handle non-finite values.
Results may differ from the reference program's by a relative error of at most 0.018.
Values may be sent and summed in bfloat16 or wider, within the bound.
A program may use at most 64 MiB of HBM per device.

```python
import math
import jax
import jax.numpy as jnp
import numpy as np
from jax import lax

D = 2048
H = 16
KVH = 8
HD = 128
FF = 4096
TOKENS = 4096
ATT = 2048


def planted_pair(key):
    query_seed = jax.random.fold_in(key, 101)
    key_seed = jax.random.fold_in(key, 202)
    query_part = jnp.clip(jax.random.normal(query_seed, (TOKENS, H * HD), jnp.float32), -6.0, 6.0)
    key_part = jnp.clip(jax.random.normal(key_seed, (TOKENS, KVH * HD), jnp.float32), -6.0, 6.0)
    return (query_part, key_part)


def draw_queries(key, part):
    return planted_pair(key)[0].astype(jnp.bfloat16)


def draw_keys(key, part):
    return planted_pair(key)[1].astype(jnp.bfloat16)


def draw_log_gates(key, part):
    order_seed = jax.random.fold_in(key, 11)
    local_seed = jax.random.fold_in(key, 12)
    fast_seed = jax.random.fold_in(key, 13)
    slow_seed = jax.random.fold_in(key, 14)
    block_seed = jax.random.fold_in(key, 15)
    head_order = jax.random.permutation(order_seed, H)
    fast = head_order < H // 2
    local = jnp.exp(0.8 * jax.random.normal(local_seed, (H, TOKENS), jnp.float32))
    fast_rate = jnp.exp(jax.random.uniform(fast_seed, (H,), jnp.float32, math.log(1.0 / 150.0), math.log(1.0 / 45.0)))
    slow_rate = jnp.exp(jax.random.uniform(slow_seed, (H,), jnp.float32, math.log(0.3), math.log(1.2))) / TOKENS
    rate = jnp.where(fast, fast_rate, slow_rate)
    block_factor = jnp.exp(jax.random.uniform(block_seed, (H, TOKENS // 64), jnp.float32, math.log(0.5), math.log(2.0)))
    stretched = jnp.repeat(block_factor, 64, axis=1)
    return -jnp.cumsum(rate[:, None] * stretched * local, axis=1)


def block_levels(key, dims, split, smallest, top_value):
    level = 1.0
    for axis_at, blocks in split:
        steps = jax.random.uniform(jax.random.fold_in(jax.random.fold_in(key, 6), axis_at), (blocks,), jnp.float32, smallest / len(split), top_value / len(split))
        level = level * jnp.repeat(jnp.exp(steps), dims[axis_at] // blocks).reshape((-1,) + (1,) * (len(dims) - 1 - axis_at))
    return level


def length_profile(count, total, reach, lean):
    weights = [(1 << 20) // math.isqrt(standing ** lean) + 1 for standing in range(2, count + 1)]
    surplus, counts = total - reach - (count - 1), [1] * (count - 1)
    while surplus > 0:
        movable = [i for i in range(count - 1) if counts[i] < reach]
        mass, left = sum([weights[i] for i in movable]), surplus
        for i in movable:
            more = min(reach - counts[i], max(1, left * weights[i] // mass), surplus)
            counts[i] = counts[i] + more
            surplus = surplus - more
    return np.array([reach] + counts)


def ragged_sizes(own_key, count, total, limit, slope):
    if count == 2:
        one = jax.random.randint(own_key, (), max(1, total - limit), min(limit, total - 1) + 1)
        return jnp.stack([one, total - one])
    tallies = jnp.asarray(length_profile(count, total, limit, slope), jnp.int32)
    pairs = (count - 1) // 2
    giver, taker = tallies[1:1 + 2 * pairs:2], tallies[2:2 + 2 * pairs:2]
    slack = jnp.minimum(giver - 1, limit - taker)
    moved = jax.random.randint(jax.random.fold_in(own_key, 1), (pairs,), 0, 1 << 20) % (slack + 1)
    tallies = tallies.at[1:1 + 2 * pairs:2].set(giver - moved).at[2:2 + 2 * pairs:2].set(taker + moved)
    return tallies[jax.random.permutation(jax.random.fold_in(own_key, 2), count)]


def centred(rng, extent, spread, most, cuts=(), held_as=jnp.bfloat16):
    level = block_levels(rng, extent, cuts, -0.22, 0.18) if cuts else 1.0
    entries = jax.random.normal(rng, extent, jnp.float32) * spread * level
    return jnp.minimum(jnp.maximum(entries, -most), most).astype(held_as)


def setup_inputs(seed: int = 0) -> dict:
    splits = jax.random.split(jax.random.key(seed), 13)
    resid = centred(splits[0], (TOKENS, D), 1.0, 6.0, ((0, 32),))
    queries = draw_queries(jax.random.fold_in(splits[12], 71), 0)
    keys = draw_keys(jax.random.fold_in(splits[12], 71), 0)
    values = centred(splits[3], (TOKENS, KVH * HD), 1.0, 6.0, ((0, 16), (1, 2)))
    log_gates = draw_log_gates(jax.random.fold_in(splits[12], 71), 0)
    documents = jnp.searchsorted(jnp.cumsum(ragged_sizes(splits[5], 3, TOKENS, TOKENS * 3 // 4, 0)), jnp.arange(TOKENS), side="right").astype(jnp.int32)
    out_weight = centred(splits[6], (ATT, D), ATT ** -0.5, 0.125, ((0, 2),))
    attn_gain = jnp.clip(1.0 + 0.18 * jax.random.normal(splits[7], (D,), jnp.float32), 0.1, 1.9)
    mlp_gain = jnp.clip(1.0 + 0.18 * jax.random.normal(splits[8], (D,), jnp.float32), 0.1, 1.9)
    gate_weight = centred(splits[9], (D, FF), D ** -0.5, 0.125, ((0, 16), (1, 2)))
    up_weight = centred(splits[10], (D, FF), D ** -0.5, 0.125, ((0, 16), (1, 2)))
    down_weight = centred(splits[11], (FF, D), (FF // 16) ** -0.5, 0.375, ((0, 2), (1, 16)))
    return dict(resid=resid, queries=queries, keys=keys, values=values, log_gates=log_gates, documents=documents, out_weight=out_weight, attn_gain=attn_gain, mlp_gain=mlp_gain, gate_weight=gate_weight, up_weight=up_weight, down_weight=down_weight)


def reference(resid, queries, keys, values, log_gates, documents, out_weight, attn_gain, mlp_gain, gate_weight, up_weight, down_weight):
    group_size = H // KVH
    score_scale = 1.0 / math.sqrt(HD)
    key_heads = keys.reshape(TOKENS, KVH, HD).astype(jnp.float32)
    value_heads = values.reshape(TOKENS, KVH, HD).astype(jnp.float32)
    key_gates = log_gates.reshape(KVH, group_size, TOKENS)
    positions = jnp.arange(TOKENS, dtype=jnp.int32)
    block_len = math.gcd(TOKENS, 512)

    def attend(block_index):
        first_row = (block_index * block_len).astype(jnp.int32)
        query_block = lax.dynamic_slice_in_dim(queries, first_row, block_len, 0)
        query_block = query_block.reshape(block_len, KVH, group_size, HD).astype(jnp.float32)
        scores = jnp.einsum('tkgd,skd->kgts', query_block, key_heads) * score_scale
        query_gates = lax.dynamic_slice_in_dim(key_gates, first_row, block_len, 2)
        scores = scores + query_gates[..., None] - key_gates[:, :, None, :]
        query_pos = first_row + jnp.arange(block_len, dtype=jnp.int32)
        query_docs = lax.dynamic_slice_in_dim(documents, first_row, block_len, 0)
        visible = (positions[None, :] <= query_pos[:, None]) & (documents[None, :] == query_docs[:, None])
        scores = jnp.where(visible, scores, jnp.float32(-1e+30))
        row_max = lax.optimization_barrier(jnp.max(scores, axis=-1, keepdims=True))
        probs = jnp.where(visible, jnp.exp(scores - row_max), jnp.float32(0.0))
        row_sum = lax.optimization_barrier(jnp.sum(probs, axis=-1))
        probs_low = probs.astype(jnp.bfloat16).astype(jnp.float32)
        summed = jnp.einsum('kgts,skd->tkgd', probs_low, value_heads)
        summed = summed / jnp.transpose(row_sum, (2, 0, 1))[..., None]
        return summed.reshape(block_len, H * HD).astype(jnp.bfloat16)
    blocks = lax.map(attend, jnp.arange(TOKENS // block_len, dtype=jnp.int32))
    attended = blocks.reshape(TOKENS, H * HD)
    projected = jnp.dot(attended, out_weight, preferred_element_type=jnp.float32)
    power = lax.optimization_barrier(jnp.mean(projected * projected, axis=-1, keepdims=True))
    middle = resid.astype(jnp.float32) + attn_gain * projected * lax.rsqrt(power + 1e-06)
    middle_power = lax.optimization_barrier(jnp.mean(middle * middle, axis=-1, keepdims=True))
    normed = (mlp_gain * middle * lax.rsqrt(middle_power + 1e-06)).astype(jnp.bfloat16)
    gate_act = jnp.dot(normed, gate_weight, preferred_element_type=jnp.float32)
    up_act = jnp.dot(normed, up_weight, preferred_element_type=jnp.float32)
    hidden = (jax.nn.silu(gate_act) * up_act).astype(jnp.bfloat16)
    lowered = jnp.dot(hidden, down_weight, preferred_element_type=jnp.float32)
    return (middle + 0.5 * lowered).astype(jnp.bfloat16)
```

```python
import functools
import math

import jax
import jax.numpy as jnp
from jax import lax
from jax.experimental import pallas as pl
from jax.experimental.pallas import tpu as pltpu
from jax.sharding import PartitionSpec as P

HD = 128


def local(
    resid,
    queries,
    keys,
    values,
    log_gates,
    documents,
    out_weight,
    attn_gain,
    mlp_gain,
    gate_weight,
    up_weight,
    down_weight,
):
    tok_rows = queries.shape[0]
    kv_dev = keys.shape[1] // HD
    heads_dev = log_gates.shape[0]
    group_size = heads_dev // kv_dev
    score_scale = 1.0 / math.sqrt(HD)
    own_start = lax.axis_index("sp") * tok_rows
    own_last = own_start + tok_rows - 1
    first_doc = documents[0]
    query_pos = own_start + lax.iota(jnp.int32, tok_rows)
    query_heads = queries.reshape(tok_rows, kv_dev, group_size, HD)
    key_gates_all = log_gates.reshape(kv_dev, group_size, log_gates.shape[1])
    query_gates = lax.dynamic_slice_in_dim(key_gates_all, own_start, tok_rows, 2)
    collected = (
        lax.all_gather(gate_weight, "sp", axis=0, tiled=True),
        lax.all_gather(up_weight, "sp", axis=0, tiled=True),
        lax.all_gather(down_weight, "sp", axis=1, tiled=True),
    )
    residual_rows = resid.astype(jnp.float32)

    def attend_block(running, key_rows, value_rows, doc_rows, first_row):
        run_max, run_sum, accumulated = running
        key_count = key_rows.shape[0]
        scores = (
            jnp.einsum(
                "tkgd,skd->kgts",
                query_heads,
                key_rows.reshape(key_count, kv_dev, HD),
                preferred_element_type=jnp.float32,
            )
            * score_scale
        )
        key_gates = lax.dynamic_slice_in_dim(key_gates_all, first_row, key_count, 2)
        scores = scores + query_gates[..., None] - key_gates[:, :, None, :]
        key_pos = first_row + lax.iota(jnp.int32, key_count)
        visible = (key_pos[None, :] <= query_pos[:, None]) & (
            doc_rows[None, :] == documents[:, None]
        )
        scores = jnp.where(visible, scores, jnp.float32(-1e30))
        new_max = jnp.maximum(run_max, jnp.max(scores, axis=-1))
        probs = jnp.where(visible, jnp.exp(scores - new_max[..., None]), jnp.float32(0.0))
        shrink = jnp.exp(run_max - new_max)
        run_sum = run_sum * shrink + jnp.sum(probs, axis=-1)
        weighted = jnp.einsum(
            "kgts,skd->kgtd",
            probs.astype(jnp.bfloat16),
            value_rows.reshape(key_count, kv_dev, HD),
            preferred_element_type=jnp.float32,
        )
        accumulated = accumulated * shrink[..., None] + weighted
        return (new_max, run_sum, accumulated)

    def maybe_attend(running, key_rows, value_rows, doc_rows, first_row):
        needed = (first_row <= own_last) & (doc_rows[-1] >= first_doc)

        def compute(state):
            return attend_block(state, key_rows, value_rows, doc_rows, first_row)

        def keep(state):
            return state

        return lax.cond(needed, compute, keep, running)

    start_state = (
        jnp.full((kv_dev, group_size, tok_rows), -1e30, jnp.float32),
        jnp.zeros((kv_dev, group_size, tok_rows), jnp.float32),
        jnp.zeros((kv_dev, group_size, tok_rows, HD), jnp.float32),
    )
    key_rows = lax.all_gather(keys, "sp", axis=0, tiled=True)
    value_rows = lax.all_gather(values, "sp", axis=0, tiled=True)
    doc_rows = lax.all_gather(documents, "sp", axis=0, tiled=True)
    key_count = key_rows.shape[0]
    block_len = math.gcd(key_count, 1024)

    def advance(block_index, inner):
        offset = block_index * block_len
        return maybe_attend(
            inner,
            lax.dynamic_slice_in_dim(key_rows, offset, block_len, 0),
            lax.dynamic_slice_in_dim(value_rows, offset, block_len, 0),
            lax.dynamic_slice_in_dim(doc_rows, offset, block_len, 0),
            offset,
        )

    run_max, run_sum, accumulated = lax.fori_loop(0, key_count // block_len, advance, start_state)
    attended = accumulated / run_sum[..., None]
    attended = (
        jnp.transpose(attended, (2, 0, 1, 3)).reshape(tok_rows, heads_dev * HD).astype(jnp.bfloat16)
    )
    rows_slice = attended
    projected = lax.psum_scatter(
        jnp.dot(rows_slice, out_weight, preferred_element_type=jnp.float32).astype(jnp.bfloat16),
        "tp",
        scatter_dimension=0,
        tiled=True,
    ).astype(jnp.float32)
    power = jnp.mean(projected * projected, axis=-1, keepdims=True)
    middle = residual_rows + attn_gain * projected * lax.rsqrt(power + 1e-06)
    middle_power = jnp.mean(middle * middle, axis=-1, keepdims=True)
    normed = (mlp_gain * middle * lax.rsqrt(middle_power + 1e-06)).astype(jnp.bfloat16)
    normed_all = lax.all_gather(normed, "tp", axis=0, tiled=True)
    gate_full, up_full, down_full = collected
    gate_act = jnp.dot(normed_all, gate_full, preferred_element_type=jnp.float32)
    up_act = jnp.dot(normed_all, up_full, preferred_element_type=jnp.float32)
    hidden = (jax.nn.silu(gate_act) * up_act).astype(jnp.bfloat16)
    rows_slice = hidden
    lowered = lax.psum_scatter(
        jnp.dot(rows_slice, down_full, preferred_element_type=jnp.float32).astype(jnp.bfloat16),
        "tp",
        scatter_dimension=0,
        tiled=True,
    ).astype(jnp.float32)
    return (middle + 0.5 * lowered).astype(jnp.bfloat16)


GROUP = 4
MESH = pl.DeviceIdType.MESH
LOG2E = 1.4426950408889634
VMEM = pl.BlockSpec(memory_space=pltpu.VMEM)


def greet(targets):
    barrier = pltpu.get_barrier_semaphore()
    for target in targets:
        pl.semaphore_signal(barrier, inc=1, device_id=target, device_id_type=MESH)
    pl.semaphore_wait(barrier, len(targets))


def remote(src, dst, send_sem, recv_sem, target):
    return pltpu.make_async_remote_copy(
        src_ref=src,
        dst_ref=dst,
        send_sem=send_sem,
        recv_sem=recv_sem,
        device_id=target,
        device_id_type=MESH,
    )


def spread_kernel(
    plane, q_ref, k_ref, v_ref, d_ref, g_ref, u_ref, w_ref,
    qo, ko, vo, do, go, uo, wo,
    z_send, p_send, recv, q_send, q_recv, local_sem,
):
    me = lax.axis_index("sp")
    core = lax.axis_index("tp")
    z, p = me // plane, me % plane
    rows = k_ref.shape[0]
    wrows = g_ref.shape[0]
    qcols = q_ref.shape[1] // GROUP
    fcols = g_ref.shape[1] // GROUP
    wcols = w_ref.shape[1]

    def cols(width, index):
        return pl.ds(pl.multiple_of(index * width, width), width)

    def place(a, k):
        if a == 0:
            return ko.at[cols(rows, k)]
        if a == 1:
            return vo.at[cols(rows, k)]
        if a == 2:
            return do.at[k]
        if a == 3:
            return go.at[cols(wrows, k)]
        if a == 4:
            return uo.at[cols(wrows, k)]
        return wo.at[:, cols(wcols, k)]

    def piece(a, to):
        if a == 0:
            return k_ref.at[:, cols(HD, to)]
        if a == 1:
            return v_ref.at[:, cols(HD, to)]
        if a == 2:
            return d_ref.at[...]
        if a == 3:
            return g_ref.at[:, cols(fcols, to)]
        if a == 4:
            return u_ref.at[:, cols(fcols, to)]
        return w_ref.at[cols(fcols, to)]

    z_peers = [(z + d) % GROUP for d in range(1, GROUP)]
    p_peers = [(p + d) % plane for d in range(1, plane)]
    greet([(t * plane + p, core) for t in z_peers] + [(z * plane + t, core) for t in p_peers])
    waits = []
    keeps = []

    def send_z(a):
        for d in range(1, GROUP):
            to = (z + d) % GROUP
            copy = remote(piece(a, to), place(a, me), z_send.at[a, d - 1],
                          recv.at[a, d, 0], (to * plane + p, core))
            copy.start()
            waits.append(copy)
        own = pltpu.make_async_copy(piece(a, z), place(a, me), local_sem.at[a])
        own.start()
        keeps.append(own)

    def forward(a, dz):
        zs = (z + GROUP - dz) % GROUP
        at = place(a, zs * plane + p)
        if dz:
            remote(at, at, z_send.at[a, dz - 1], recv.at[a, dz, 0], (me, core)).wait_recv()
        else:
            keeps[a].wait()
        for e in range(1, plane):
            copy = remote(at, at, p_send.at[a, dz, e - 1], recv.at[a, dz, e],
                          (z * plane + (p + e) % plane, core))
            copy.start()
            waits.append(copy)

    for a in (0, 1, 2):
        send_z(a)
    for d in range(1, GROUP):
        to = (z + d) % GROUP
        copy = remote(q_ref.at[:, cols(qcols, to)], qo.at[z], q_send.at[d - 1],
                      q_recv.at[d - 1], (to * plane + p, core))
        copy.start()
        waits.append(copy)
    own_q = pltpu.make_async_copy(q_ref.at[:, cols(qcols, z)], qo.at[z], local_sem.at[6])
    own_q.start()
    for a in (3, 4, 5):
        send_z(a)
    for group in ((0, 1, 2), (3, 4, 5)):
        for dz in (0, 1, 3, 2):
            for a in group:
                forward(a, dz)
    own_q.wait()
    for copy in waits:
        copy.wait_send()
    for d in range(1, GROUP):
        at = qo.at[(z + GROUP - d) % GROUP]
        remote(at, at, q_send.at[d - 1], q_recv.at[d - 1], (me, core)).wait_recv()
    for a in range(6):
        for dz in range(GROUP):
            zs = (z + GROUP - dz) % GROUP
            for e in range(1, plane):
                at = place(a, zs * plane + (p + plane - e) % plane)
                remote(at, at, p_send.at[a, dz, e - 1], recv.at[a, dz, e], (me, core)).wait_recv()


def attend_kernel(lo_ref, hi_ref, q_ref, k_ref, v_ref, gq_ref, gk_ref, dq_ref, dk_ref, pos_ref,
                  out_ref):
    block = 512
    rows = q_ref.shape[1]
    rank = q_ref.shape[2] // HD
    coef = LOG2E / math.sqrt(HD)

    def one(b, carry):
        q = jnp.concatenate([q_ref[b, :, r * HD:(r + 1) * HD] for r in range(rank)], axis=0)
        dq = dq_ref[b]
        qpos = pos_ref[b]
        gq = gq_ref[b]

        def step(i, state):
            m, l, acc = state
            at = pl.ds(pl.multiple_of(i * block, block), block)
            s = lax.dot_general(q, k_ref[at], (((1,), (1,)), ((), ())),
                                preferred_element_type=jnp.float32)
            gk = jnp.concatenate(
                [jnp.broadcast_to(gk_ref[r:r + 1, at], (rows, block)) for r in range(rank)], axis=0)
            s = s * coef + (gq - gk)
            kpos = i * block + lax.broadcasted_iota(jnp.int32, (1, block), 1)
            seen = (kpos <= qpos) & (dk_ref[0:1, at] == dq)
            s = jnp.where(seen, s, jnp.float32(-1e30))
            m_new = jnp.maximum(m, jnp.max(s, axis=1, keepdims=True))
            prob = jnp.exp2(s - m_new)
            shrink = jnp.exp2(m - m_new)
            l = l * shrink + jnp.sum(prob, axis=1, keepdims=True)
            acc = acc * shrink + jnp.dot(prob.astype(jnp.bfloat16), v_ref[at],
                                         preferred_element_type=jnp.float32)
            return m_new, l, acc

        start = (jnp.full((rank * rows, 1), -1e20, jnp.float32),
                 jnp.zeros((rank * rows, 1), jnp.float32),
                 jnp.zeros((rank * rows, HD), jnp.float32))
        m, l, acc = lax.fori_loop(lo_ref[b], hi_ref[b], step, start)
        res = (acc / l).astype(jnp.bfloat16)
        for r in range(rank):
            out_ref[b, :, r * HD:(r + 1) * HD] = res[r * rows:(r + 1) * rows]
        return carry

    lax.fori_loop(0, q_ref.shape[0], one, 0)


def finish_kernel(
    plane, att_ref, ow_ref, resid_ref, ag_ref, mg_ref, gw_ref, uw_ref, dw_ref, out_ref,
    arr, pbuf, pgot, mid, nall, hid, part, pair, red, got,
    a_send, a_recv, t_send, t_recv, n_send, n_recv, f_send, f_recv,
    x_send, x_recv, r_send, r_recv, local_sem,
):
    me = lax.axis_index("sp")
    core = lax.axis_index("tp")
    z, p = me // plane, me % plane
    other = 1 - core
    mate = (me, other)
    width = att_ref.shape[2]
    half = resid_ref.shape[0]
    d_model = resid_ref.shape[1]
    tile = 512

    def there(d):
        return (((z + d) % GROUP) * plane + p, core)

    greet([there(d) for d in range(1, GROUP)] + [mate])
    for d in range(1, GROUP):
        remote(att_ref.at[(z + d) % GROUP], arr.at[z], a_send.at[d - 1], a_recv.at[d - 1],
               there(d)).start()
    own = pltpu.make_async_copy(att_ref.at[z], arr.at[z], local_sem)
    own.start()
    own.wait()
    for d in range(1, GROUP):
        at = arr.at[(z + GROUP - d) % GROUP]
        remote(at, at, a_send.at[d - 1], a_recv.at[d - 1], mate).wait_recv()

    @pl.loop(0, d_model // tile)
    def _(j):
        at = pl.ds(pl.multiple_of(j * tile, tile), tile)
        total = jnp.dot(arr[0], ow_ref[0:width, at], preferred_element_type=jnp.float32)
        for g in range(1, GROUP):
            total += jnp.dot(arr[g], ow_ref[g * width:(g + 1) * width, at],
                             preferred_element_type=jnp.float32)
        pbuf[0, :, at] = total[:half].astype(jnp.bfloat16)
        pbuf[1, :, at] = total[half:].astype(jnp.bfloat16)

    swap = remote(pbuf.at[other], pgot, t_send, t_recv, mate)
    swap.start()
    swap.wait()
    projected = pbuf[core].astype(jnp.float32) + pgot[...].astype(jnp.float32)
    power = jnp.mean(projected * projected, axis=-1, keepdims=True)
    middle = resid_ref[...].astype(jnp.float32) + ag_ref[...] * projected * lax.rsqrt(power + 1e-06)
    mid[...] = middle
    mpower = jnp.mean(middle * middle, axis=-1, keepdims=True)
    nall[z, core] = (mg_ref[...] * middle * lax.rsqrt(mpower + 1e-06)).astype(jnp.bfloat16)
    mine = nall.at[z, core]
    for d in range(1, GROUP):
        remote(mine, mine, n_send.at[d - 1], n_recv.at[d - 1], there(d)).start()
    remote(mine, mine, f_send.at[0], f_recv.at[0], mate).start()

    for d in (0, 1, 3, 2):
        zb = (z + GROUP - d) % GROUP
        here, over = nall.at[zb, core], nall.at[zb, other]
        if d:
            remote(here, here, n_send.at[d - 1], n_recv.at[d - 1], mate).wait_recv()
            remote(here, here, f_send.at[d], f_recv.at[d], mate).start()
        remote(over, over, f_send.at[d], f_recv.at[d], mate).wait_recv()
        rows_in = jnp.concatenate([nall[zb, 0], nall[zb, 1]], axis=0)
        ftile = 256
        for j in range(hid.shape[1] // ftile):
            at = slice(j * ftile, (j + 1) * ftile)
            gate = jnp.dot(rows_in, gw_ref[:, at], preferred_element_type=jnp.float32)
            up = jnp.dot(rows_in, uw_ref[:, at], preferred_element_type=jnp.float32)
            hid[:, at] = (gate / (1.0 + jnp.exp(-gate)) * up).astype(jnp.bfloat16)

        @pl.loop(0, d_model // tile)
        def _(j):
            at = pl.ds(pl.multiple_of(j * tile, tile), tile)
            total = jnp.dot(hid[...], dw_ref[:, at], preferred_element_type=jnp.float32)
            part[d, 0, :, at] = total[:half].astype(jnp.bfloat16)
            part[d, 1, :, at] = total[half:].astype(jnp.bfloat16)

        trade = remote(part.at[d, other], pair.at[d], x_send.at[d], x_recv.at[d], mate)
        trade.start()
        trade.wait()
        both = part[d, core].astype(jnp.float32) + pair[d].astype(jnp.float32)
        if d:
            red[d - 1] = both.astype(jnp.bfloat16)
            remote(red.at[d - 1], got.at[d - 1], r_send.at[d - 1], r_recv.at[d - 1],
                   there(GROUP - d)).start()
        else:
            mid[...] += 0.5 * both

    total = mid[...]
    for d in range(1, GROUP):
        at = got.at[d - 1]
        remote(at, at, r_send.at[d - 1], r_recv.at[d - 1], mate).wait_recv()
        total += 0.5 * got[d - 1].astype(jnp.float32)
    out_ref[...] = total.astype(jnp.bfloat16)
    for d in range(1, GROUP):
        at = arr.at[0]
        remote(att_ref.at[0], at, a_send.at[d - 1], a_recv.at[d - 1], mate).wait_send()
        remote(mine, mine, n_send.at[d - 1], n_recv.at[d - 1], mate).wait_send()
        remote(red.at[d - 1], got.at[d - 1], r_send.at[d - 1], r_recv.at[d - 1], mate).wait_send()
    for d in range(GROUP):
        here = nall.at[(z + GROUP - d) % GROUP, core]
        remote(here, here, f_send.at[d], f_recv.at[d], mate).wait_send()


def grouped(
    sp, resid, queries, keys, values, log_gates, documents, out_weight, attn_gain, mlp_gain,
    gate_weight, up_weight, down_weight,
):
    plane = sp // GROUP
    rows, ff = keys.shape[0], gate_weight.shape[1] // GROUP
    d_model = resid.shape[1]
    tokens = rows * sp
    qcols = queries.shape[1] // GROUP
    rank = qcols // HD
    bf = jnp.bfloat16
    me = lax.axis_index("sp")
    z, p = me // plane, me % plane
    shape = jax.ShapeDtypeStruct
    dma = pltpu.SemaphoreType.DMA
    limit = 60 * 1024 * 1024
    q4, k_all, v_all, docs, g_all, u_all, w_all = pl.pallas_call(
        functools.partial(spread_kernel, plane),
        out_shape=(
            shape((GROUP, rows, qcols), bf), shape((tokens, HD), bf), shape((tokens, HD), bf),
            shape((sp, 8, rows), jnp.int32),
            shape((d_model, ff), bf), shape((d_model, ff), bf), shape((ff, d_model), bf),
        ),
        in_specs=[VMEM] * 7,
        out_specs=[VMEM] * 7,
        scratch_shapes=[
            dma((6, GROUP - 1)), dma((6, GROUP, plane - 1)), dma((6, GROUP, plane)),
            dma((GROUP - 1,)), dma((GROUP - 1,)), dma((7,)),
        ],
        compiler_params=pltpu.CompilerParams(
            collective_id=0, has_side_effects=True, vmem_limit_bytes=limit),
    )(queries, keys, values, jnp.broadcast_to(documents[None, :], (8, rows)),
      gate_weight, up_weight, down_weight)

    docs_all = docs[:, 0, :].reshape(tokens)
    gates = lax.dynamic_slice_in_dim(log_gates, z * rank, rank, 0) * LOG2E
    def mine(x):
        return lax.dynamic_index_in_dim(x, p, x.ndim - 2, keepdims=False)
    gq = mine(gates.reshape(rank, GROUP, plane, rows))
    gq = jnp.transpose(gq, (1, 0, 2)).reshape(GROUP, rank * rows, 1)
    dq = mine(docs_all.reshape(GROUP, plane, rows))
    pos = mine(lax.iota(jnp.int32, tokens).reshape(GROUP, plane, rows))
    block = 512
    hi = (pos[:, -1] + block) // block
    lo = jnp.sum((docs_all[None, :] < dq[:, :1]).astype(jnp.int32), axis=1) // block
    SMEM = pl.BlockSpec(memory_space=pltpu.SMEM)
    attended = pl.pallas_call(
        attend_kernel,
        out_shape=shape((GROUP, rows, qcols), bf),
        in_specs=[SMEM, SMEM] + [VMEM] * 8,
        out_specs=VMEM,
        compiler_params=pltpu.CompilerParams(vmem_limit_bytes=limit),
    )(lo, hi, q4, k_all, v_all, gq, gates, jnp.tile(dq, (1, rank))[..., None],
      docs_all[None, :], jnp.tile(pos, (1, rank))[..., None])

    half = resid.shape[0]
    return pl.pallas_call(
        functools.partial(finish_kernel, plane),
        out_shape=shape(resid.shape, bf),
        in_specs=[VMEM] * 8,
        out_specs=VMEM,
        scratch_shapes=[
            pltpu.VMEM((GROUP, rows, qcols), bf),
            pltpu.VMEM((2, half, d_model), bf),
            pltpu.VMEM((half, d_model), bf),
            pltpu.VMEM((half, d_model), jnp.float32),
            pltpu.VMEM((GROUP, 2, half, d_model), bf),
            pltpu.VMEM((rows, ff), bf),
            pltpu.VMEM((GROUP, 2, half, d_model), bf),
            pltpu.VMEM((GROUP, half, d_model), bf),
            pltpu.VMEM((GROUP - 1, half, d_model), bf),
            pltpu.VMEM((GROUP - 1, half, d_model), bf),
            dma((GROUP - 1,)), dma((GROUP - 1,)), dma, dma,
            dma((GROUP - 1,)), dma((GROUP - 1,)), dma((GROUP,)), dma((GROUP,)),
            dma((GROUP,)), dma((GROUP,)), dma((GROUP - 1,)), dma((GROUP - 1,)), dma,
        ],
        compiler_params=pltpu.CompilerParams(
            collective_id=1, has_side_effects=True, vmem_limit_bytes=limit),
    )(attended, out_weight, resid, attn_gain[None, :], mlp_gain[None, :], g_all, u_all, w_all)


def solution(mesh):
    placed = (
        P(("sp", "tp"), None),
        P("sp", "tp"),
        P("sp", "tp"),
        P("sp", "tp"),
        P("tp", None),
        P("sp"),
        P("tp", None),
        P(),
        P(),
        P("sp", "tp"),
        P("sp", "tp"),
        P("tp", "sp"),
    )
    sp, tp = mesh.shape["sp"], mesh.shape["tp"]

    def layer(*args):
        kv_dev = args[2].shape[1] // HD
        fits = tp == 2 and sp % GROUP == 0 and kv_dev == GROUP
        return grouped(sp, *args) if fits else local(*args)

    return jax.shard_map(
        layer, mesh=mesh, in_specs=placed, out_specs=P(("sp", "tp"), None), check_vma=False
    )
```

```python
import functools
import math

import jax
import jax.numpy as jnp
from jax import lax
from jax.experimental import pallas as pl
from jax.experimental.pallas import tpu as pltpu
from jax.sharding import PartitionSpec as P

HD = 128


def local(
    resid,
    queries,
    keys,
    values,
    log_gates,
    documents,
    out_weight,
    attn_gain,
    mlp_gain,
    gate_weight,
    up_weight,
    down_weight,
):
    tok_rows = queries.shape[0]
    kv_dev = keys.shape[1] // HD
    heads_dev = log_gates.shape[0]
    group_size = heads_dev // kv_dev
    score_scale = 1.0 / math.sqrt(HD)
    own_start = lax.axis_index("sp") * tok_rows
    own_last = own_start + tok_rows - 1
    first_doc = documents[0]
    query_pos = own_start + lax.iota(jnp.int32, tok_rows)
    query_heads = queries.reshape(tok_rows, kv_dev, group_size, HD)
    key_gates_all = log_gates.reshape(kv_dev, group_size, log_gates.shape[1])
    query_gates = lax.dynamic_slice_in_dim(key_gates_all, own_start, tok_rows, 2)
    collected = (
        lax.all_gather(gate_weight, "sp", axis=0, tiled=True),
        lax.all_gather(up_weight, "sp", axis=0, tiled=True),
        lax.all_gather(down_weight, "sp", axis=1, tiled=True),
    )
    residual_rows = resid.astype(jnp.float32)

    def attend_block(running, key_rows, value_rows, doc_rows, first_row):
        run_max, run_sum, accumulated = running
        key_count = key_rows.shape[0]
        scores = (
            jnp.einsum(
                "tkgd,skd->kgts",
                query_heads,
                key_rows.reshape(key_count, kv_dev, HD),
                preferred_element_type=jnp.float32,
            )
            * score_scale
        )
        key_gates = lax.dynamic_slice_in_dim(key_gates_all, first_row, key_count, 2)
        scores = scores + query_gates[..., None] - key_gates[:, :, None, :]
        key_pos = first_row + lax.iota(jnp.int32, key_count)
        visible = (key_pos[None, :] <= query_pos[:, None]) & (
            doc_rows[None, :] == documents[:, None]
        )
        scores = jnp.where(visible, scores, jnp.float32(-1e30))
        new_max = jnp.maximum(run_max, jnp.max(scores, axis=-1))
        probs = jnp.where(visible, jnp.exp(scores - new_max[..., None]), jnp.float32(0.0))
        shrink = jnp.exp(run_max - new_max)
        run_sum = run_sum * shrink + jnp.sum(probs, axis=-1)
        weighted = jnp.einsum(
            "kgts,skd->kgtd",
            probs.astype(jnp.bfloat16),
            value_rows.reshape(key_count, kv_dev, HD),
            preferred_element_type=jnp.float32,
        )
        accumulated = accumulated * shrink[..., None] + weighted
        return (new_max, run_sum, accumulated)

    def maybe_attend(running, key_rows, value_rows, doc_rows, first_row):
        needed = (first_row <= own_last) & (doc_rows[-1] >= first_doc)

        def compute(state):
            return attend_block(state, key_rows, value_rows, doc_rows, first_row)

        def keep(state):
            return state

        return lax.cond(needed, compute, keep, running)

    start_state = (
        jnp.full((kv_dev, group_size, tok_rows), -1e30, jnp.float32),
        jnp.zeros((kv_dev, group_size, tok_rows), jnp.float32),
        jnp.zeros((kv_dev, group_size, tok_rows, HD), jnp.float32),
    )
    key_rows = lax.all_gather(keys, "sp", axis=0, tiled=True)
    value_rows = lax.all_gather(values, "sp", axis=0, tiled=True)
    doc_rows = lax.all_gather(documents, "sp", axis=0, tiled=True)
    key_count = key_rows.shape[0]
    block_len = math.gcd(key_count, 1024)

    def advance(block_index, inner):
        offset = block_index * block_len
        return maybe_attend(
            inner,
            lax.dynamic_slice_in_dim(key_rows, offset, block_len, 0),
            lax.dynamic_slice_in_dim(value_rows, offset, block_len, 0),
            lax.dynamic_slice_in_dim(doc_rows, offset, block_len, 0),
            offset,
        )

    run_max, run_sum, accumulated = lax.fori_loop(0, key_count // block_len, advance, start_state)
    attended = accumulated / run_sum[..., None]
    attended = (
        jnp.transpose(attended, (2, 0, 1, 3)).reshape(tok_rows, heads_dev * HD).astype(jnp.bfloat16)
    )
    rows_slice = attended
    projected = lax.psum_scatter(
        jnp.dot(rows_slice, out_weight, preferred_element_type=jnp.float32).astype(jnp.bfloat16),
        "tp",
        scatter_dimension=0,
        tiled=True,
    ).astype(jnp.float32)
    power = jnp.mean(projected * projected, axis=-1, keepdims=True)
    middle = residual_rows + attn_gain * projected * lax.rsqrt(power + 1e-06)
    middle_power = jnp.mean(middle * middle, axis=-1, keepdims=True)
    normed = (mlp_gain * middle * lax.rsqrt(middle_power + 1e-06)).astype(jnp.bfloat16)
    normed_all = lax.all_gather(normed, "tp", axis=0, tiled=True)
    gate_full, up_full, down_full = collected
    gate_act = jnp.dot(normed_all, gate_full, preferred_element_type=jnp.float32)
    up_act = jnp.dot(normed_all, up_full, preferred_element_type=jnp.float32)
    hidden = (jax.nn.silu(gate_act) * up_act).astype(jnp.bfloat16)
    rows_slice = hidden
    lowered = lax.psum_scatter(
        jnp.dot(rows_slice, down_full, preferred_element_type=jnp.float32).astype(jnp.bfloat16),
        "tp",
        scatter_dimension=0,
        tiled=True,
    ).astype(jnp.float32)
    return (middle + 0.5 * lowered).astype(jnp.bfloat16)


GROUP = 4
MESH = pl.DeviceIdType.MESH
LOG2E = 1.4426950408889634
VMEM = pl.BlockSpec(memory_space=pltpu.VMEM)


def greet(targets):
    barrier = pltpu.get_barrier_semaphore()
    for target in targets:
        pl.semaphore_signal(barrier, inc=1, device_id=target, device_id_type=MESH)
    pl.semaphore_wait(barrier, len(targets))


def remote(src, dst, send_sem, recv_sem, target):
    return pltpu.make_async_remote_copy(
        src_ref=src,
        dst_ref=dst,
        send_sem=send_sem,
        recv_sem=recv_sem,
        device_id=target,
        device_id_type=MESH,
    )


def spread_kernel(
    plane, q_ref, k_ref, v_ref, d_ref, g_ref, u_ref, w_ref,
    qo, ko, vo, do, go, uo, wo,
    z_send, p_send, recv, q_send, q_recv, local_sem,
):
    me = lax.axis_index("sp")
    core = lax.axis_index("tp")
    z, p = me // plane, me % plane
    rows = k_ref.shape[0]
    qcols = q_ref.shape[1] // GROUP
    fcols = g_ref.shape[1] // GROUP

    def cols(width, index):
        return pl.ds(pl.multiple_of(index * width, width), width)

    def place(a, k):
        if a == 0:
            return ko.at[cols(rows, k)]
        if a == 1:
            return vo.at[cols(rows, k)]
        if a == 2:
            return do.at[k]
        if a == 3:
            return go.at[cols(g_ref.shape[0], k)]
        return (uo, wo)[a - 4].at[k // plane]

    def piece(a, to):
        if a == 0:
            return k_ref.at[:, cols(HD, to)]
        if a == 1:
            return v_ref.at[:, cols(HD, to)]
        if a == 2:
            return d_ref.at[...]
        if a == 3:
            return g_ref.at[:, cols(fcols, to)]
        if a == 4:
            return u_ref.at[:, cols(fcols, to)]
        return w_ref.at[cols(fcols, to)]

    z_peers = [(z + d) % GROUP for d in range(1, GROUP)]
    p_peers = [(p + d) % plane for d in range(1, plane)]
    greet([(t * plane + p, core) for t in z_peers] + [(z * plane + t, core) for t in p_peers])
    waits = []
    keeps = []

    def send_z(a):
        for d in range(1, GROUP):
            to = (z + d) % GROUP
            copy = remote(piece(a, to), place(a, me), z_send.at[a, d - 1],
                          recv.at[a, d, 0], (to * plane + p, core))
            copy.start()
            waits.append(copy)
        own = pltpu.make_async_copy(piece(a, z), place(a, me), local_sem.at[a])
        own.start()
        keeps.append(own)

    def forward(a, dz):
        zs = (z + GROUP - dz) % GROUP
        at = place(a, zs * plane + p)
        if dz:
            remote(at, at, z_send.at[a, dz - 1], recv.at[a, dz, 0], (me, core)).wait_recv()
        else:
            keeps[a].wait()
        for e in range(1, plane):
            copy = remote(at, at, p_send.at[a, dz, e - 1], recv.at[a, dz, e],
                          (z * plane + (p + e) % plane, core))
            copy.start()
            waits.append(copy)

    for a in (0, 1, 2):
        send_z(a)
    for d in range(1, GROUP):
        to = (z + d) % GROUP
        copy = remote(q_ref.at[:, cols(qcols, to)], qo.at[z], q_send.at[d - 1],
                      q_recv.at[d - 1], (to * plane + p, core))
        copy.start()
        waits.append(copy)
    own_q = pltpu.make_async_copy(q_ref.at[:, cols(qcols, z)], qo.at[z], local_sem.at[6])
    own_q.start()
    for a in (3, 4, 5):
        send_z(a)
    for group in ((0, 1, 2), (3,)):
        for dz in (0, 1, 3, 2):
            for a in group:
                forward(a, dz)
    for a in (4, 5):
        keeps[a].wait()
        for d in range(1, GROUP):
            at = place(a, ((z + GROUP - d) % GROUP) * plane + p)
            remote(at, at, z_send.at[a, d - 1], recv.at[a, d, 0], (me, core)).wait_recv()
    own_q.wait()
    for copy in waits:
        copy.wait_send()
    for d in range(1, GROUP):
        at = qo.at[(z + GROUP - d) % GROUP]
        remote(at, at, q_send.at[d - 1], q_recv.at[d - 1], (me, core)).wait_recv()
    for a in range(4):
        for dz in range(GROUP):
            zs = (z + GROUP - dz) % GROUP
            for e in range(1, plane):
                at = place(a, zs * plane + (p + plane - e) % plane)
                remote(at, at, p_send.at[a, dz, e - 1], recv.at[a, dz, e], (me, core)).wait_recv()


def attend_kernel(lo_ref, hi_ref, q_ref, k_ref, v_ref, gq_ref, gk_ref, dq_ref, dk_ref, pos_ref,
                  out_ref):
    block = 512
    rows = q_ref.shape[1]
    rank = q_ref.shape[2] // HD
    coef = LOG2E / math.sqrt(HD)

    def one(b, carry):
        q = jnp.concatenate([q_ref[b, :, r * HD:(r + 1) * HD] for r in range(rank)], axis=0)
        dq = dq_ref[b]
        qpos = pos_ref[b]
        gq = gq_ref[b]

        def step(i, state):
            m, l, acc = state
            at = pl.ds(pl.multiple_of(i * block, block), block)
            s = lax.dot_general(q, k_ref[at], (((1,), (1,)), ((), ())),
                                preferred_element_type=jnp.float32)
            gk = jnp.concatenate(
                [jnp.broadcast_to(gk_ref[r:r + 1, at], (rows, block)) for r in range(rank)], axis=0)
            s = s * coef + (gq - gk)
            kpos = i * block + lax.broadcasted_iota(jnp.int32, (1, block), 1)
            seen = (kpos <= qpos) & (dk_ref[0:1, at] == dq)
            s = jnp.where(seen, s, jnp.float32(-1e30))
            m_new = jnp.maximum(m, jnp.max(s, axis=1, keepdims=True))
            prob = jnp.exp2(s - m_new)
            shrink = jnp.exp2(m - m_new)
            l = l * shrink + jnp.sum(prob, axis=1, keepdims=True)
            acc = acc * shrink + jnp.dot(prob.astype(jnp.bfloat16), v_ref[at],
                                         preferred_element_type=jnp.float32)
            return m_new, l, acc

        start = (jnp.full((rank * rows, 1), -1e20, jnp.float32),
                 jnp.zeros((rank * rows, 1), jnp.float32),
                 jnp.zeros((rank * rows, HD), jnp.float32))
        m, l, acc = lax.fori_loop(lo_ref[b], hi_ref[b], step, start)
        res = (acc / l).astype(jnp.bfloat16)
        for r in range(rank):
            out_ref[b, :, r * HD:(r + 1) * HD] = res[r * rows:(r + 1) * rows]
        return carry

    lax.fori_loop(0, q_ref.shape[0], one, 0)


def finish_kernel(
    plane, att_ref, ow_ref, resid_ref, ag_ref, mg_ref, gw, uz_ref, wz_ref, out_ref,
    uw, dw, arr, pbuf, pgot, mid, nall, hid, part, pair, red, got,
    a_send, a_recv, t_send, t_recv, o_send, n_send, n_recv, f_send, f_recv,
    x_send, x_recv, r_send, r_recv, w_send, w_recv, w_local, local_sem,
):
    me = lax.axis_index("sp")
    core = lax.axis_index("tp")
    z, p = me // plane, me % plane
    other = 1 - core
    mate = (me, other)
    width = att_ref.shape[2]
    half = resid_ref.shape[0]
    d_model = resid_ref.shape[1]
    wrows, wcols = uz_ref.shape[1], wz_ref.shape[2]
    tile = 512

    def there(d):
        return (((z + d) % GROUP) * plane + p, core)

    def near(e):
        return (z * plane + (p + e) % plane, core)

    def weight(a, k):
        if a == 0:
            return uw.at[pl.ds(pl.multiple_of(k * wrows, wrows), wrows)]
        return dw.at[:, pl.ds(pl.multiple_of(k * wcols, wcols), wcols)]

    greet([there(d) for d in range(1, GROUP)] + [near(e) for e in range(1, plane)] + [mate])
    for d in range(1, GROUP):
        remote(att_ref.at[(z + d) % GROUP], arr.at[z], a_send.at[d - 1], a_recv.at[d - 1],
               there(d)).start()
    own = pltpu.make_async_copy(att_ref.at[z], arr.at[z], local_sem)
    own.start()
    staged = (uz_ref, wz_ref)
    for a in range(2):
        for g in range(GROUP):
            at = weight(a, g * plane + p)
            pltpu.make_async_copy(staged[a].at[g], at, w_local.at[a, g]).start()
            for e in range(1, plane):
                remote(staged[a].at[g], at, w_send.at[a, g, e - 1], w_recv.at[a, g, e - 1],
                       near(e)).start()
    own.wait()
    for d in range(1, GROUP):
        at = arr.at[(z + GROUP - d) % GROUP]
        remote(at, at, a_send.at[d - 1], a_recv.at[d - 1], mate).wait_recv()

    @pl.loop(0, d_model // tile)
    def _(j):
        at = pl.ds(pl.multiple_of(j * tile, tile), tile)
        total = jnp.dot(arr[0], ow_ref[0:width, at], preferred_element_type=jnp.float32)
        for g in range(1, GROUP):
            total += jnp.dot(arr[g], ow_ref[g * width:(g + 1) * width, at],
                             preferred_element_type=jnp.float32)
        pbuf[0, :, at] = total[:half].astype(jnp.bfloat16)
        pbuf[1, :, at] = total[half:].astype(jnp.bfloat16)

    swap = remote(pbuf.at[other], pgot, t_send, t_recv, mate)
    swap.start()
    swap.wait()
    projected = pbuf[core].astype(jnp.float32) + pgot[...].astype(jnp.float32)
    power = jnp.mean(projected * projected, axis=-1, keepdims=True)
    middle = resid_ref[...].astype(jnp.float32) + ag_ref[...] * projected * lax.rsqrt(power + 1e-06)
    mid[...] = middle
    mpower = jnp.mean(middle * middle, axis=-1, keepdims=True)
    nall[z, core] = (mg_ref[...] * middle * lax.rsqrt(mpower + 1e-06)).astype(jnp.bfloat16)

    def relay(zb, side, send_sem):
        block = nall.at[zb, core]
        return remote(block, block, send_sem, n_recv.at[zb],
                      ((z + 1 - 2 * side) * plane + p, core))

    def share(zb):
        block = nall.at[zb, core]
        return remote(block, block, f_send.at[zb], f_recv.at[zb], mate)

    def onward(side):
        return (side == 0) & (z < GROUP - 1) | (side == 1) & (z > 0)

    for side in (0, 1):
        @pl.when(onward(side))
        def _():
            relay(z, side, o_send.at[side]).start()
    share(z).start()

    def feed(zb):
        over = nall.at[zb, other]
        remote(over, over, f_send.at[zb], f_recv.at[zb], mate).wait_recv()
        rows_in = jnp.concatenate([nall[zb, 0], nall[zb, 1]], axis=0)
        ftile = 256
        for j in range(hid.shape[1] // ftile):
            at = slice(j * ftile, (j + 1) * ftile)
            gate = jnp.dot(rows_in, gw[:, at], preferred_element_type=jnp.float32)
            up = jnp.dot(rows_in, uw[:, at], preferred_element_type=jnp.float32)
            hid[:, at] = (gate / (1.0 + jnp.exp(-gate)) * up).astype(jnp.bfloat16)

        @pl.loop(0, d_model // tile)
        def _(j):
            at = pl.ds(pl.multiple_of(j * tile, tile), tile)
            total = jnp.dot(hid[...], dw[:, at], preferred_element_type=jnp.float32)
            part[zb, 0, :, at] = total[:half].astype(jnp.bfloat16)
            part[zb, 1, :, at] = total[half:].astype(jnp.bfloat16)

        trade = remote(part.at[zb, other], pair.at[zb], x_send.at[zb], x_recv.at[zb], mate)
        trade.start()
        trade.wait()
        return part[zb, core].astype(jnp.float32) + pair[zb].astype(jnp.float32)

    def arrive(d):
        for side in (0, 1):
            zb = z - d if side == 0 else z + d

            @pl.when((zb >= 0) & (zb < GROUP))
            def _():
                block = nall.at[zb, core]
                remote(block, block, n_send.at[zb], n_recv.at[zb], mate).wait_recv()
                @pl.when(onward(side))
                def _():
                    relay(zb, side, n_send.at[zb]).start()
                share(zb).start()

    arrive(1)
    arrive(2)
    for a in range(2):
        for g in range(GROUP):
            pltpu.make_async_copy(staged[a].at[g], weight(a, g * plane + p),
                                  w_local.at[a, g]).wait()
            for e in range(1, plane):
                at = weight(a, g * plane + (p + plane - e) % plane)
                remote(staged[a].at[g], at, w_send.at[a, g, e - 1], w_recv.at[a, g, e - 1],
                       near(e)).wait()
    for d in (2, 1, 3):
        if d == 3:
            arrive(d)

        @pl.loop(0, 2)
        def _(side):
            zb = z + (2 * side - 1) * d

            @pl.when((zb >= 0) & (zb < GROUP))
            def _():
                red[zb] = feed(zb).astype(jnp.bfloat16)
                remote(red.at[zb], got.at[z], r_send.at[zb], r_recv.at[z],
                       (zb * plane + p, core)).start()
    total = mid[...] + 0.5 * feed(z)
    for d in range(1, GROUP):
        zb = (z + d) % GROUP
        remote(red.at[zb], got.at[zb], r_send.at[zb], r_recv.at[zb], mate).wait()
        total += 0.5 * got[zb].astype(jnp.float32)
    out_ref[...] = total.astype(jnp.bfloat16)
    share(z).wait_send()
    for side in (0, 1):
        @pl.when(onward(side))
        def _():
            relay(z, side, o_send.at[side]).wait_send()
    for d in range(1, GROUP):
        remote(att_ref.at[0], arr.at[0], a_send.at[d - 1], a_recv.at[d - 1], mate).wait_send()
        share((z + d) % GROUP).wait_send()
        for side in (0, 1):
            zb = z - d if side == 0 else z + d

            @pl.when((zb >= 0) & (zb < GROUP) & onward(side))
            def _():
                relay(zb, side, n_send.at[zb]).wait_send()


def grouped(
    sp, resid, queries, keys, values, log_gates, documents, out_weight, attn_gain, mlp_gain,
    gate_weight, up_weight, down_weight,
):
    plane = sp // GROUP
    rows, ff = keys.shape[0], gate_weight.shape[1] // GROUP
    d_model = resid.shape[1]
    wrows, wcols = gate_weight.shape[0], down_weight.shape[1]
    tokens = rows * sp
    qcols = queries.shape[1] // GROUP
    rank = qcols // HD
    bf = jnp.bfloat16
    me = lax.axis_index("sp")
    z, p = me // plane, me % plane
    shape = jax.ShapeDtypeStruct
    dma = pltpu.SemaphoreType.DMA
    limit = 60 * 1024 * 1024
    q4, k_all, v_all, docs, g_all, u_all, w_all = pl.pallas_call(
        functools.partial(spread_kernel, plane),
        out_shape=(
            shape((GROUP, rows, qcols), bf), shape((tokens, HD), bf), shape((tokens, HD), bf),
            shape((sp, 8, rows), jnp.int32),
            shape((d_model, ff), bf), shape((GROUP, wrows, ff), bf),
            shape((GROUP, ff, wcols), bf),
        ),
        in_specs=[VMEM] * 7,
        out_specs=[VMEM] * 7,
        scratch_shapes=[
            dma((6, GROUP - 1)), dma((6, GROUP, plane - 1)), dma((6, GROUP, plane)),
            dma((GROUP - 1,)), dma((GROUP - 1,)), dma((7,)),
        ],
        compiler_params=pltpu.CompilerParams(
            collective_id=0, has_side_effects=True, vmem_limit_bytes=limit),
    )(queries, keys, values, jnp.broadcast_to(documents[None, :], (8, rows)),
      gate_weight, up_weight, down_weight)

    docs_all = docs[:, 0, :].reshape(tokens)
    gates = lax.dynamic_slice_in_dim(log_gates, z * rank, rank, 0) * LOG2E
    def mine(x):
        return lax.dynamic_index_in_dim(x, p, x.ndim - 2, keepdims=False)
    gq = mine(gates.reshape(rank, GROUP, plane, rows))
    gq = jnp.transpose(gq, (1, 0, 2)).reshape(GROUP, rank * rows, 1)
    dq = mine(docs_all.reshape(GROUP, plane, rows))
    pos = mine(lax.iota(jnp.int32, tokens).reshape(GROUP, plane, rows))
    block = 512
    hi = (pos[:, -1] + block) // block
    lo = jnp.sum((docs_all[None, :] < dq[:, :1]).astype(jnp.int32), axis=1) // block
    SMEM = pl.BlockSpec(memory_space=pltpu.SMEM)
    attended = pl.pallas_call(
        attend_kernel,
        out_shape=shape((GROUP, rows, qcols), bf),
        in_specs=[SMEM, SMEM] + [VMEM] * 8,
        out_specs=VMEM,
        compiler_params=pltpu.CompilerParams(vmem_limit_bytes=limit),
    )(lo, hi, q4, k_all, v_all, gq, gates, jnp.tile(dq, (1, rank))[..., None],
      docs_all[None, :], jnp.tile(pos, (1, rank))[..., None])

    half = resid.shape[0]
    return pl.pallas_call(
        functools.partial(finish_kernel, plane),
        out_shape=shape(resid.shape, bf),
        in_specs=[VMEM] * 8,
        out_specs=VMEM,
        scratch_shapes=[
            pltpu.VMEM((d_model, ff), bf),
            pltpu.VMEM((ff, d_model), bf),
            pltpu.VMEM((GROUP, rows, qcols), bf),
            pltpu.VMEM((2, half, d_model), bf),
            pltpu.VMEM((half, d_model), bf),
            pltpu.VMEM((half, d_model), jnp.float32),
            pltpu.VMEM((GROUP, 2, half, d_model), bf),
            pltpu.VMEM((rows, ff), bf),
            pltpu.VMEM((GROUP, 2, half, d_model), bf),
            pltpu.VMEM((GROUP, half, d_model), bf),
            pltpu.VMEM((GROUP, half, d_model), bf),
            pltpu.VMEM((GROUP, half, d_model), bf),
            dma((GROUP - 1,)), dma((GROUP - 1,)), dma, dma,
            dma((2,)), dma((GROUP,)), dma((GROUP,)), dma((GROUP,)), dma((GROUP,)),
            dma((GROUP,)), dma((GROUP,)), dma((GROUP,)), dma((GROUP,)),
            dma((2, GROUP, plane - 1)), dma((2, GROUP, plane - 1)), dma((2, GROUP)), dma,
        ],
        compiler_params=pltpu.CompilerParams(
            collective_id=1, has_side_effects=True, vmem_limit_bytes=limit),
    )(attended, out_weight, resid, attn_gain[None, :], mlp_gain[None, :], g_all, u_all, w_all)


def solution(mesh):
    placed = (
        P(("sp", "tp"), None),
        P("sp", "tp"),
        P("sp", "tp"),
        P("sp", "tp"),
        P("tp", None),
        P("sp"),
        P("tp", None),
        P(),
        P(),
        P("sp", "tp"),
        P("sp", "tp"),
        P("tp", "sp"),
    )
    sp, tp = mesh.shape["sp"], mesh.shape["tp"]

    def layer(*args):
        kv_dev = args[2].shape[1] // HD
        fits = tp == 2 and sp % GROUP == 0 and kv_dev == GROUP
        return grouped(sp, *args) if fits else local(*args)

    return jax.shard_map(
        layer, mesh=mesh, in_specs=placed, out_specs=P(("sp", "tp"), None), check_vma=False
    )
```
